32 devices in a mesh: sp: 16 (over z, y, x), tp: 2 (over core).
Axes of the slice: x: 2, y: 2, z: 4, core: 2. Of those that a mesh axis runs over, the one named last changes fastest.
Arguments:
- residual_in: bfloat16 [8192, 2048], P(('sp', 'tp')), may hold values from -6 to 6
- queries: bfloat16 [8192, 2048], P('sp', 'tp'), may hold values from -200 to 200
- keys: bfloat16 [8192, 512], P('sp', 'tp'), may hold values from -5.5 to 5.5
- values: bfloat16 [8192, 512], P('sp', 'tp'), may hold values from -6 to 6
- docs: int32 [8192], P('sp'), may hold values from 0 to 3, never falling along the last dimension, each value on 1 to 4096 neighbouring positions
- sink: float32 [32], P('tp'), may hold values from 1 to 7
- out_weight: bfloat16 [2048, 2048], P('tp'), may hold values from -0.125 to 0.125
- gate_weight: bfloat16 [2048, 5632], P('sp', 'tp'), may hold values from -0.125 to 0.125
- up_weight: bfloat16 [2048, 5632], P('sp', 'tp'), may hold values from -0.125 to 0.125
- down_weight: bfloat16 [5632, 2048], P('tp', 'sp'), may hold values from -0.078125 to 0.078125
- conv_taps: float32 [3, 5632], P(None, 'tp'), may hold values from -3.5 to 3.5
- norm_gains: float32 [3, 2048], replicated, may hold values from 0.1 to 1.9
Outputs:
- layer_out: bfloat16 [8192, 2048], P(('sp', 'tp'))
The draws below stay inside these ranges and needn't reach their ends.
All inputs are finite; a program needn't handle non-finite values.
Results may differ from the reference program's by a relative error of at most 0.02.
Values may be sent and summed in bfloat16 or wider, within the bound.
No kernel may reach another device: no remote copies, remote signals or barrier semaphores. Data moves between devices by JAX's collectives and lax.ppermute only.
A program may use at most 128 MiB of HBM per device.

```python
import math
import jax
import jax.numpy as jnp
import numpy as np
from jax import lax

D = 2048
HEADS = 32
KV_HEADS = 8
HEAD = 64
FF = 5632
WINDOW = 128
TOK_DEV = 512
TOKENS = 8192
N_SP = 16
N_TP = 2


def base_keys(key):
    drawn = jax.random.normal(jax.random.fold_in(key, 11), (TOKENS, KV_HEADS * HEAD), jnp.float32)
    return jnp.clip(drawn, -5.5, 5.5)


def draw_keys(key, part):
    return base_keys(key).astype(jnp.bfloat16)


def draw_queries(key, part):
    drawn = jax.random.normal(jax.random.fold_in(key, 12), (TOKENS, HEADS * HEAD), jnp.float32)
    drawn = jnp.clip(drawn, -5.5, 5.5)
    return drawn.astype(jnp.bfloat16)


def level_of(key, dims, cuts, least, top_value):
    factor_of = 1.0
    for dim, shards_of in cuts:
        heights = jax.random.uniform(jax.random.fold_in(jax.random.fold_in(key, 6), dim), (shards_of,), jnp.float32, least / len(cuts), top_value / len(cuts))
        factor_of = factor_of * jnp.repeat(jnp.exp(heights), dims[dim] // shards_of).reshape((-1,) + (1,) * (len(dims) - 1 - dim))
    return factor_of


def length_profile(amount, total, bound, slope):
    portions = [(1 << 20) // math.isqrt(standing ** slope) + 1 for standing in range(2, amount + 1)]
    surplus, counts = total - bound - (amount - 1), [1] * (amount - 1)
    while surplus > 0:
        free = [i for i in range(amount - 1) if counts[i] < bound]
        pool, remaining = sum([portions[i] for i in free]), surplus
        for i in free:
            extra = min(bound - counts[i], max(1, remaining * portions[i] // pool), surplus)
            counts[i] = counts[i] + extra
            surplus = surplus - extra
    return np.array([bound] + counts)


def uneven_parts(rng, number_of, total, most, lean):
    if number_of == 2:
        one = jax.random.randint(rng, (), max(1, total - most), min(most, total - 1) + 1)
        return jnp.stack([one, total - one])
    tallies = jnp.asarray(length_profile(number_of, total, most, lean), jnp.int32)
    pairs = (number_of - 1) // 2
    giver, taker = tallies[1:1 + 2 * pairs:2], tallies[2:2 + 2 * pairs:2]
    room = jnp.minimum(giver - 1, most - taker)
    passed = jax.random.randint(jax.random.fold_in(rng, 1), (pairs,), 0, 1 << 20) % (room + 1)
    tallies = tallies.at[1:1 + 2 * pairs:2].set(giver - passed).at[2:2 + 2 * pairs:2].set(taker + passed)
    return tallies[jax.random.permutation(jax.random.fold_in(rng, 2), number_of)]


def noise(stream_key, dims, deviation, bound, shards=(), held_as=jnp.bfloat16):
    entries = deviation * jax.random.normal(stream_key, dims, jnp.float32)
    if shards:
        entries = entries * level_of(stream_key, dims, shards, -0.22, 0.18)
    return jnp.clip(entries, -bound, bound).astype(held_as)


def setup_inputs(seed: int = 0) -> dict:
    splits = jax.random.split(jax.random.key(seed), 13)
    return {
        "residual_in": noise(splits[0], (TOKENS, D), 1.0, 6.0, ((0, 32),)),
        "queries": draw_queries(jax.random.fold_in(splits[12], 71), 0),
        "keys": draw_keys(jax.random.fold_in(splits[12], 71), 0),
        "values": noise(splits[3], (TOKENS, KV_HEADS * HEAD), 1.0, 6.0, ((0, 16), (1, 2))),
        "docs": jnp.searchsorted(jnp.cumsum(uneven_parts(splits[4], N_SP // 4, TOKENS, 8 * TOK_DEV, 1)), jnp.arange(TOKENS), side="right").astype(jnp.int32),
        "sink": jnp.clip(1.0 + 6.0 * jax.random.uniform(splits[5], (HEADS,), jnp.float32) ** level_of(splits[5], (HEADS,), ((0, 2),), -0.2, 0.2), 1.0, 7.0),
        "out_weight": noise(splits[6], (HEADS * HEAD, D), (HEADS * HEAD) ** -0.5, 0.125, ((0, 2),)),
        "gate_weight": noise(splits[7], (D, FF), D ** -0.5, 0.125, ((0, 16), (1, 2))),
        "up_weight": noise(splits[8], (D, FF), D ** -0.5, 0.125, ((0, 16), (1, 2))),
        "down_weight": noise(splits[9], (FF, D), FF ** -0.5, 0.078125, ((0, 2), (1, 16))),
        "conv_taps": noise(splits[10], (3, FF), 3 ** -0.5, 3.5, ((1, 2),), jnp.float32),
        "norm_gains": jnp.clip(1.0 + 0.18 * jax.random.normal(splits[11], (3, D), jnp.float32), 0.1, 1.9),
    }


rope_base = 10000.0
neg_large = -1e+30
norm_eps = 1e-06

def rotate(block, positions):
    rows = block.shape[0]
    heads = block.shape[1] // HEAD
    half = HEAD // 2
    freq = rope_base ** (-jnp.arange(half, dtype=jnp.float32) * 2.0 / HEAD)
    angle = positions.astype(jnp.float32)[:, None] * freq[None, :]
    cosine = jnp.cos(angle)[:, None, :]
    sine = jnp.sin(angle)[:, None, :]
    shaped = block.astype(jnp.float32).reshape(rows, heads, 2, half)
    first = shaped[:, :, 0]
    second = shaped[:, :, 1]
    turned = jnp.stack([first * cosine - second * sine, second * cosine + first * sine], axis=2)
    return turned.reshape(rows, heads * HEAD).astype(jnp.bfloat16)

def attend(queries, keys, values, allowed, sink):
    rows = queries.shape[0]
    kv_local = keys.shape[1] // HEAD
    group = queries.shape[1] // HEAD // kv_local
    shaped_q = queries.astype(jnp.float32).reshape(rows, kv_local, group, HEAD)
    shaped_k = keys.astype(jnp.float32).reshape(keys.shape[0], kv_local, HEAD)
    shaped_v = values.astype(jnp.float32).reshape(values.shape[0], kv_local, HEAD)
    scores = jnp.einsum('qngd,knd->ngqk', shaped_q, shaped_k) * HEAD ** (-0.5)
    scores = jnp.where(allowed[None, None], scores, neg_large)
    sink_group = sink.reshape(kv_local, group)[:, :, None]
    top = jnp.maximum(lax.optimization_barrier(jnp.max(scores, axis=-1)), sink_group)
    weights = jnp.exp(scores - top[..., None])
    total = lax.optimization_barrier(jnp.sum(weights, axis=-1)) + jnp.exp(sink_group - top)
    probs = (weights / total[..., None]).astype(jnp.bfloat16)
    out = jnp.einsum('ngqk,knd->qngd', probs.astype(jnp.float32), shaped_v)
    return out.reshape(rows, kv_local * group * HEAD).astype(jnp.bfloat16)

def normalize(vector, gain):
    scale = lax.rsqrt(lax.optimization_barrier(jnp.mean(vector * vector, axis=-1, keepdims=True)) + norm_eps)
    return vector * scale * gain

def reference(residual_in, queries, keys, values, docs, sink, out_weight, gate_weight, up_weight, down_weight, conv_taps, norm_gains):
    positions = jnp.arange(TOKENS, dtype=jnp.int32)
    q_rot = rotate(queries, positions)
    k_rot = rotate(keys, positions)
    pad_keys = jnp.pad(k_rot, ((WINDOW, WINDOW), (0, 0)))
    pad_values = jnp.pad(values, ((WINDOW, WINDOW), (0, 0)))
    pad_docs = jnp.pad(docs, (WINDOW, WINDOW), constant_values=-1)
    span = TOK_DEV + 2 * WINDOW

    def one_block(index):
        start = (index * TOK_DEV).astype(jnp.int32)
        q_blk = lax.dynamic_slice_in_dim(q_rot, start, TOK_DEV, 0)
        k_blk = lax.dynamic_slice_in_dim(pad_keys, start, span, 0)
        v_blk = lax.dynamic_slice_in_dim(pad_values, start, span, 0)
        d_blk = lax.dynamic_slice_in_dim(pad_docs, start, span, 0)
        own = lax.dynamic_slice_in_dim(docs, start, TOK_DEV, 0)
        here = start + jnp.arange(TOK_DEV, dtype=jnp.int32)
        there = start - WINDOW + jnp.arange(span, dtype=jnp.int32)
        allowed = (jnp.abs(there[None, :] - here[:, None]) <= WINDOW) & (d_blk[None, :] == own[:, None])
        return attend(q_blk, k_blk, v_blk, allowed, sink)
    attended = lax.map(one_block, jnp.arange(N_SP, dtype=jnp.int32)).reshape(TOKENS, HEADS * HEAD)
    part = HEADS * HEAD // N_TP
    mixed = jnp.zeros((TOKENS, D), jnp.float32)
    for index in range(N_TP):
        term = jnp.dot(attended[:, index * part:(index + 1) * part], out_weight[index * part:(index + 1) * part], preferred_element_type=jnp.float32).astype(jnp.bfloat16)
        mixed = mixed + lax.optimization_barrier(term).astype(jnp.float32)
    updated = (residual_in.astype(jnp.float32) + normalize(mixed, norm_gains[0])).astype(jnp.bfloat16)
    normed = normalize(updated.astype(jnp.float32), norm_gains[1]).astype(jnp.bfloat16)
    pad_normed = jnp.pad(normed, ((1, 1), (0, 0)))
    pad_near = jnp.pad(docs, (1, 1), constant_values=-1)
    width = FF // N_TP

    def ffn_block(index):
        start = (index * TOK_DEV).astype(jnp.int32)
        rows_ext = lax.dynamic_slice_in_dim(pad_normed, start, TOK_DEV + 2, 0)
        gate_low = jnp.dot(rows_ext, gate_weight, preferred_element_type=jnp.float32).astype(jnp.bfloat16)
        gate = lax.optimization_barrier(gate_low).astype(jnp.float32)
        up = jnp.dot(rows_ext[1:-1], up_weight, preferred_element_type=jnp.float32)
        near = lax.dynamic_slice_in_dim(pad_near, start, TOK_DEV + 2, 0)
        own = near[1:-1]
        same_prev = (near[:-2] == own)[:, None]
        same_next = (near[2:] == own)[:, None]
        conv = conv_taps[0] * jnp.where(same_prev, gate[:-2], 0.0) + conv_taps[1] * gate[1:-1] + conv_taps[2] * jnp.where(same_next, gate[2:], 0.0)
        hidden = (jax.nn.silu(conv) * up).astype(jnp.bfloat16)
        total = jnp.zeros((TOK_DEV, D), jnp.float32)
        for group in range(N_TP):
            term = jnp.dot(hidden[:, group * width:(group + 1) * width], down_weight[group * width:(group + 1) * width], preferred_element_type=jnp.float32).astype(jnp.bfloat16)
            total = total + lax.optimization_barrier(term).astype(jnp.float32)
        return total
    ffn_out = lax.map(ffn_block, jnp.arange(N_SP, dtype=jnp.int32)).reshape(TOKENS, D)
    return (updated.astype(jnp.float32) + normalize(ffn_out, norm_gains[2])).astype(jnp.bfloat16)
```

```python
import jax
import jax.numpy as jnp
from jax import lax
from jax.sharding import PartitionSpec as P

HEAD = 64
WINDOW = 128
X, Y, ZL = 1, 2, 4
FAR = 8

rope_base = 10000.0
neg_large = -1e30
norm_eps = 1e-06


def rotate(block, positions):
    rows = block.shape[0]
    heads = block.shape[1] // HEAD
    half = HEAD // 2
    freq = rope_base ** (-jnp.arange(half, dtype=jnp.float32) * 2.0 / HEAD)
    angle = positions.astype(jnp.float32)[:, None] * freq[None, :]
    cosine = jnp.cos(angle)[:, None, :]
    sine = jnp.sin(angle)[:, None, :]
    shaped = block.astype(jnp.float32).reshape(rows, heads, 2, half)
    first = shaped[:, :, 0]
    second = shaped[:, :, 1]
    turned = jnp.stack([first * cosine - second * sine, second * cosine + first * sine], axis=2)
    return turned.reshape(rows, heads * HEAD).astype(jnp.bfloat16)


def attend(queries, keys, values, allowed, sink):
    rows = queries.shape[0]
    kv_local = keys.shape[1] // HEAD
    group = queries.shape[1] // HEAD // kv_local
    shaped_q = queries.reshape(rows, kv_local, group, HEAD)
    shaped_k = keys.reshape(keys.shape[0], kv_local, HEAD)
    shaped_v = values.reshape(values.shape[0], kv_local, HEAD)
    scores = jnp.einsum(
        "qngd,knd->ngqk", shaped_q, shaped_k, preferred_element_type=jnp.float32
    ) * HEAD ** (-0.5)
    scores = jnp.where(allowed[None, None], scores, neg_large)
    sink_group = sink.reshape(kv_local, group)[:, :, None]
    top = jnp.maximum(jnp.max(scores, axis=-1), sink_group)
    weights = jnp.exp(scores - top[..., None])
    total = jnp.sum(weights, axis=-1) + jnp.exp(sink_group - top)
    probs = (weights / total[..., None]).astype(jnp.bfloat16)
    out = jnp.einsum("ngqk,knd->qngd", probs, shaped_v, preferred_element_type=jnp.float32)
    return out.reshape(rows, kv_local * group * HEAD).astype(jnp.bfloat16)


def normalize(vector, gain):
    scale = lax.rsqrt(jnp.mean(vector * vector, axis=-1, keepdims=True) + norm_eps)
    return vector * scale * gain


def swap(cells, bit):
    return lax.ppermute(cells, "sp", [(i, i ^ bit) for i in range(lax.axis_size("sp"))])


def pair(at, mine, other):
    return jnp.where(at == 0, jnp.stack([mine, other]), jnp.stack([other, mine]))


def pick(cells, index, axis):
    return lax.dynamic_index_in_dim(cells, index, axis, keepdims=False)


class Place:
    def __init__(self):
        self.me = lax.axis_index("sp")
        self.core = lax.axis_index("tp")
        self.count = lax.axis_size("sp")
        self.cores = lax.axis_size("tp")
        self.x = self.me & 1
        self.y = (self.me >> 1) & 1
        self.zl = (self.me >> 2) & 1
        self.far = self.me >> 3
        self.fars = self.count // FAR


def spread(at, parts):
    kept = pick(parts, at.x, 1)
    came = swap(pick(parts, 1 - at.x, 1), X)
    both = pair(at.x, kept, came)
    kept = pick(both, at.zl, 1)
    came = swap(pick(both, 1 - at.zl, 1), ZL)
    four = pair(at.zl, kept, came)
    cells = four.shape[2:]
    whole = jnp.zeros((at.fars, 2, 2, 2) + cells, four.dtype)

    def put(whole, block, far, y):
        zero = jnp.zeros((), jnp.int32)
        start = (far, zero, y, zero) + (zero,) * len(cells)
        return lax.dynamic_update_slice(whole, block[None, :, None], start)

    distant = [(0, four)]
    for step in range(1, at.fars):
        shift = [(i, (i + step * FAR) % at.count) for i in range(at.count)]
        distant.append((step, lax.ppermute(four, "sp", shift)))
    for step, block in distant:
        far = lax.rem(at.far - step + at.fars, at.fars)
        whole = put(whole, block, far, at.y)
        whole = put(whole, swap(block, Y), far, 1 - at.y)
    return whole


def core_gather(at, block):
    whole = jnp.zeros((at.cores,) + block.shape, block.dtype)
    rest = (jnp.zeros((), jnp.int32),) * block.ndim
    for step in range(at.cores):
        came = block
        if step:
            shift = [(i, (i + step) % at.cores) for i in range(at.cores)]
            came = lax.ppermute(block, "tp", shift)
        owner = lax.rem(at.core - step + at.cores, at.cores)
        whole = lax.dynamic_update_slice(whole, came[None], (owner,) + rest)
    return whole


def core_scatter(at, blocks, axis):
    total = pick(blocks, at.core, axis).astype(jnp.float32)
    for step in range(1, at.cores):
        shift = [(i, (i + step) % at.cores) for i in range(at.cores)]
        sent = pick(blocks, lax.rem(at.core + step, at.cores), axis)
        total = total + lax.ppermute(sent, "tp", shift).astype(jnp.float32)
    return total


def local(
    residual_in,
    queries,
    keys,
    values,
    docs,
    sink,
    out_weight,
    gate_weight,
    up_weight,
    down_weight,
    conv_taps,
    norm_gains,
):
    at = Place()
    rows = queries.shape[0]
    own = residual_in.shape[0]
    width = residual_in.shape[1]
    hidden_part = gate_weight.shape[1] // 4
    depth = gate_weight.shape[0]
    low = jnp.bfloat16
    full = jnp.float32

    def columns(weight):
        parts = [weight[:, i * hidden_part : (i + 1) * hidden_part] for i in range(4)]
        return jnp.stack(parts).reshape(2, 2, depth, hidden_part)

    gate_whole = spread(at, columns(gate_weight)).reshape(width, hidden_part)
    up_whole = spread(at, columns(up_weight)).reshape(width, hidden_part)
    down_whole = spread(at, down_weight.reshape(2, 2, hidden_part, depth))
    down_whole = down_whole.reshape(at.count, hidden_part, depth)
    down_whole = jnp.swapaxes(down_whole, 0, 1).reshape(hidden_part, width)

    offset = at.me * rows
    total_len = at.count * rows
    near = jnp.concatenate(
        [keys, values, jnp.broadcast_to(docs.astype(low)[:, None], (rows, 128))], axis=1
    )
    ends = at.count - 1
    before = lax.ppermute(near[rows - WINDOW :], "sp", [(i, i + 1) for i in range(ends)])
    after = lax.ppermute(near[:WINDOW], "sp", [(i + 1, i) for i in range(ends)])
    near = jnp.concatenate([before, near, after], axis=0)
    kv = keys.shape[1]
    keys_ext = near[:, :kv]
    values_ext = near[:, kv : 2 * kv]
    docs_ext = near[:, 2 * kv].astype(jnp.int32)
    here = offset + jnp.arange(rows, dtype=jnp.int32)
    there = offset - WINDOW + jnp.arange(rows + 2 * WINDOW, dtype=jnp.int32)
    q_rot = rotate(queries, here)
    k_rot = rotate(keys_ext, there)
    allowed = (
        (jnp.abs(there[None, :] - here[:, None]) <= WINDOW)
        & (there[None, :] >= 0)
        & (there[None, :] < total_len)
        & (docs_ext[None, :] == docs[:, None])
    )
    attended = attend(q_rot, k_rot, values_ext, allowed, sink)
    term = jnp.dot(attended, out_weight, preferred_element_type=full).astype(low)
    mixed = core_scatter(at, term.reshape(at.cores, own, width), 0)
    updated = (residual_in.astype(full) + normalize(mixed, norm_gains[0])).astype(low)
    normed = normalize(updated.astype(full), norm_gains[1]).astype(low)

    inside = (there >= 0) & (there < total_len)
    linked = jnp.where(inside, docs_ext, -1)
    same_prev = linked[WINDOW - 1 : WINDOW - 1 + rows] == docs
    same_next = linked[WINDOW + 1 : WINDOW + 1 + rows] == docs
    code = same_prev.astype(low) + 2 * same_next.astype(low)
    code = pick(code.reshape(at.cores, own), at.core, 0)
    code = jnp.pad(code[None], ((0, 15), (0, width - own)))
    packed = jnp.concatenate([normed, code], axis=0)
    two = pair(at.zl, packed, swap(packed, ZL))
    four = pair(at.x, two, swap(two, X))
    tokens = core_gather(at, four)
    tokens = tokens.transpose(2, 1, 0, 3, 4)
    codes = tokens[:, :, :, own, :own].reshape(2, 2 * rows, 1)
    same_prev = (codes == 1) | (codes == 3)
    same_next = codes >= 2
    ffn_in = tokens[:, :, :, :own].reshape(4 * rows, width)

    gate = jnp.dot(ffn_in, gate_whole, preferred_element_type=full).astype(low)
    gate = gate.reshape(2, 2 * rows, hidden_part)
    edges = jnp.stack([gate[:, 0], gate[:, -1]], axis=1)
    side = swap(edges, Y)
    hops = []
    for i in range(at.count):
        goal = i - Y + FAR if i & Y else i + Y - FAR
        if 0 <= goal < at.count:
            hops.append((i, goal))
    beyond = lax.ppermute(jnp.where(at.y == 1, edges[1, 1], edges[0, 0]), "sp", hops)
    previous = jnp.where(
        at.y == 1, jnp.stack([side[0, 1], side[1, 1]]), jnp.stack([beyond, side[0, 1]])
    )
    following = jnp.where(
        at.y == 1, jnp.stack([side[1, 0], beyond]), jnp.stack([side[0, 0], side[1, 0]])
    )
    up = jnp.dot(ffn_in, up_whole, preferred_element_type=full).reshape(gate.shape)
    gate_ext = jnp.concatenate([previous[:, None], gate, following[:, None]], axis=1).astype(full)
    taps = pick(conv_taps.reshape(3, 4, hidden_part), at.zl * 2 + at.x, 1)
    conv = (
        taps[0] * jnp.where(same_prev, gate_ext[:, :-2], 0.0)
        + taps[1] * gate_ext[:, 1:-1]
        + taps[2] * jnp.where(same_next, gate_ext[:, 2:], 0.0)
    )
    hidden = (jax.nn.silu(conv) * up).astype(low).reshape(4 * rows, hidden_part)
    terms = jnp.dot(hidden, down_whole, preferred_element_type=full).astype(low)
    terms = core_scatter(at, terms.reshape(2, 2, at.cores, own, width), 2)
    low_terms = terms.astype(low)
    sums = pick(terms, at.x, 1) + swap(pick(low_terms, 1 - at.x, 1), X).astype(full)
    low_sums = sums.astype(low)
    ffn_out = pick(sums, at.zl, 0) + swap(pick(low_sums, 1 - at.zl, 0), ZL).astype(full)
    return (updated.astype(full) + normalize(ffn_out, norm_gains[2])).astype(low)


def solution(mesh):
    in_specs = (
        P(("sp", "tp"), None),
        P("sp", "tp"),
        P("sp", "tp"),
        P("sp", "tp"),
        P("sp"),
        P("tp"),
        P("tp", None),
        P("sp", "tp"),
        P("sp", "tp"),
        P("tp", "sp"),
        P(None, "tp"),
        P(),
    )
    out_specs = P(("sp", "tp"), None)
    return jax.shard_map(local, mesh=mesh, in_specs=in_specs, out_specs=out_specs, check_vma=False)
```

```python
import jax
import jax.numpy as jnp
from jax import lax
from jax.experimental import pallas as pl
from jax.experimental.pallas import tpu as pltpu
from jax.sharding import PartitionSpec as P


HEAD = 64
WINDOW = 128


rope_base = 10000.0
neg_large = -1e30
norm_eps = 1e-06


def padded(cells, sides, width):
    for axis, dim in sides:
        count = lax.axis_size(axis)
        ends = count - 1
        head = lax.slice_in_dim(cells, 0, width, axis=dim)
        tail = lax.slice_in_dim(cells, cells.shape[dim] - width, cells.shape[dim], axis=dim)
        cells = jnp.concatenate(
            [
                lax.ppermute(tail, axis, [(i, (i + 1) % count) for i in range(ends)]),
                cells,
                lax.ppermute(head, axis, [((i + 1) % count, i) for i in range(ends)]),
            ],
            axis=dim,
        )
    return cells


def rotate(block, positions):
    rows = block.shape[0]
    heads = block.shape[1] // HEAD
    half = HEAD // 2
    freq = rope_base ** (-jnp.arange(half, dtype=jnp.float32) * 2.0 / HEAD)
    angle = positions.astype(jnp.float32)[:, None] * freq[None, :]
    cosine = jnp.cos(angle)[:, None, :]
    sine = jnp.sin(angle)[:, None, :]
    shaped = block.astype(jnp.float32).reshape(rows, heads, 2, half)
    first = shaped[:, :, 0]
    second = shaped[:, :, 1]
    turned = jnp.stack([first * cosine - second * sine, second * cosine + first * sine], axis=2)
    return turned.reshape(rows, heads * HEAD).astype(jnp.bfloat16)


def attend(queries, keys, values, allowed, sink):
    rows = queries.shape[0]
    kv_local = keys.shape[1] // HEAD
    group = queries.shape[1] // HEAD // kv_local
    shaped_q = queries.reshape(rows, kv_local, group, HEAD)
    shaped_k = keys.reshape(keys.shape[0], kv_local, HEAD)
    shaped_v = values.reshape(values.shape[0], kv_local, HEAD)
    scores = jnp.einsum(
        "qngd,knd->ngqk", shaped_q, shaped_k, preferred_element_type=jnp.float32
    ) * HEAD ** (-0.5)
    scores = jnp.where(allowed[None, None], scores, neg_large)
    sink_group = sink.reshape(kv_local, group)[:, :, None]
    top = jnp.maximum(jnp.max(scores, axis=-1), sink_group)
    weights = jnp.exp(scores - top[..., None])
    total = jnp.sum(weights, axis=-1) + jnp.exp(sink_group - top)
    probs = (weights / total[..., None]).astype(jnp.bfloat16)
    out = jnp.einsum("ngqk,knd->qngd", probs, shaped_v, preferred_element_type=jnp.float32)
    return out.reshape(rows, kv_local * group * HEAD).astype(jnp.bfloat16)


def normalize(vector, gain):
    scale = lax.rsqrt(jnp.mean(vector * vector, axis=-1, keepdims=True) + norm_eps)
    return vector * scale * gain


def plain(
    residual_in,
    queries,
    keys,
    values,
    docs,
    sink,
    out_weight,
    gate_weight,
    up_weight,
    down_weight,
    conv_taps,
    norm_gains,
):
    rows = queries.shape[0]
    offset = lax.axis_index("sp") * rows
    total_len = lax.axis_size("sp") * rows
    keys_ext, values_ext, docs_ext = (
        padded(keys, (("sp", 0),), WINDOW),
        padded(values, (("sp", 0),), WINDOW),
        padded(docs, (("sp", 0),), WINDOW),
    )
    here = offset + jnp.arange(rows, dtype=jnp.int32)
    there = offset - WINDOW + jnp.arange(rows + 2 * WINDOW, dtype=jnp.int32)
    q_rot = rotate(queries, here)
    k_rot = rotate(keys_ext, there)
    allowed = (
        (jnp.abs(there[None, :] - here[:, None]) <= WINDOW)
        & (there[None, :] >= 0)
        & (there[None, :] < total_len)
        & (docs_ext[None, :] == docs[:, None])
    )
    attended = attend(q_rot, k_rot, values_ext, allowed, sink)
    mixed = lax.psum_scatter(
        jnp.dot(attended, out_weight, preferred_element_type=jnp.float32).astype(jnp.bfloat16),
        "tp",
        scatter_dimension=0,
        tiled=True,
    ).astype(jnp.float32)
    updated = (residual_in.astype(jnp.float32) + normalize(mixed, norm_gains[0])).astype(
        jnp.bfloat16
    )
    normed = normalize(updated.astype(jnp.float32), norm_gains[1]).astype(jnp.bfloat16)
    ffn_in = lax.all_gather(normed, "tp", axis=0, tiled=True)
    gate = jnp.dot(
        ffn_in,
        lax.all_gather(gate_weight, "sp", axis=0, tiled=True),
        preferred_element_type=jnp.float32,
    )
    up = jnp.dot(
        ffn_in,
        lax.all_gather(up_weight, "sp", axis=0, tiled=True),
        preferred_element_type=jnp.float32,
    )
    gate_low = gate.astype(jnp.bfloat16)
    gate_ext = padded(gate_low, (("sp", 0),), 1).astype(jnp.float32)
    same_prev = (docs_ext[WINDOW - 1 : WINDOW - 1 + rows] == docs)[:, None]
    same_next = (docs_ext[WINDOW + 1 : WINDOW + 1 + rows] == docs)[:, None]
    conv = (
        conv_taps[0] * jnp.where(same_prev, gate_ext[:-2], 0.0)
        + conv_taps[1] * gate_ext[1:-1]
        + conv_taps[2] * jnp.where(same_next, gate_ext[2:], 0.0)
    )
    hidden = (jax.nn.silu(conv) * up).astype(jnp.bfloat16)
    terms = jnp.dot(
        hidden,
        lax.all_gather(down_weight, "sp", axis=1, tiled=True),
        preferred_element_type=jnp.float32,
    )
    ffn_out = lax.psum_scatter(
        terms.astype(jnp.bfloat16), "tp", scatter_dimension=0, tiled=True
    ).astype(jnp.float32)
    return (updated.astype(jnp.float32) + normalize(ffn_out, norm_gains[2])).astype(jnp.bfloat16)


LANES = 128
X, Y, ZL, FAR = 1, 2, 4, 8
low = jnp.bfloat16
full = jnp.float32
params = pltpu.CompilerParams(vmem_limit_bytes=60 * 1024 * 1024)


def hbm():
    return pl.BlockSpec(memory_space=pl.ANY)


def vmem():
    return pl.BlockSpec(memory_space=pltpu.VMEM)


def smem():
    return pl.BlockSpec(memory_space=pltpu.SMEM)


def cost(flops, bytes_accessed):
    return pl.CostEstimate(flops=flops, bytes_accessed=bytes_accessed, transcendentals=0)


def swap(cells, bit):
    return lax.ppermute(cells, "sp", [(i, i ^ bit) for i in range(lax.axis_size("sp"))])


def pick(cells, index, axis):
    return lax.dynamic_index_in_dim(cells, index, axis, keepdims=False)


class Place:
    def __init__(self):
        self.me = lax.axis_index("sp")
        self.core = lax.axis_index("tp")
        self.count = lax.axis_size("sp")
        self.cores = lax.axis_size("tp")
        self.x = self.me & 1
        self.y = (self.me >> 1) & 1
        self.zl = (self.me >> 2) & 1
        self.fars = self.count // FAR

    def other_core(self, cells):
        return lax.ppermute(cells, "tp", [(i, i ^ 1) for i in range(self.cores)])

    def far_shift(self, cells, step):
        hops = [(i, (i + step * FAR) % self.count) for i in range(self.count)]
        return lax.ppermute(cells, "sp", hops)


def exchange(at, parts):
    kept = pick(parts, at.x, 1)
    came = swap(pick(parts, 1 - at.x, 1), X)
    sent = jnp.stack([pick(kept, 1 - at.zl, 0), pick(came, 1 - at.zl, 0)])
    mine = jnp.stack([pick(kept, at.zl, 0), pick(came, at.zl, 0)])
    return jnp.concatenate([mine, swap(sent, ZL)])


def spread(at, parts):
    four = exchange(at, parts)
    pieces = [(0, 0, four), (0, 1, swap(four, Y))]
    for step in range(1, at.fars):
        away = at.far_shift(four, step)
        pieces += [(step, 0, away), (step, 1, swap(away, Y))]
    return pieces


OFFSETS = (0, X, ZL, X | ZL)


def shard_of(me, fars, step, y, slot):
    near = (me & 7) ^ (OFFSETS[slot] | (Y if y else 0))
    return near + FAR * lax.rem((me >> 3) - step + fars, fars)


def load_rows(me, spots, refs, whole, sems, depth, fars):
    copies = []
    for (step, y), ref in zip(spots, refs):
        for slot in range(4):
            shard = shard_of(me, fars, step, y, slot)
            rows = pl.ds(pl.multiple_of(shard * depth, depth), depth)
            copies.append(
                pltpu.make_async_copy(ref.at[slot], whole.at[rows], sems.at[len(copies)])
            )
    for copy in copies:
        copy.start()
    return copies


def attend_body(half_ref, sink_ref, q_ref, near_ref, cos_ref, sin_ref, weight_ref, out_ref, kd, vd, held):
    kv = held.shape[1] // 4
    span = kd.shape[1]
    rows = held.shape[0]
    step = WINDOW
    window = 3 * step
    start = pl.multiple_of(half_ref[0] * rows, rows)
    lane = lax.broadcasted_iota(jnp.int32, (1, LANES), 1)
    front = lane % HEAD < HEAD // 2
    left = lane < HEAD

    def rotated(cells, cosine, sine):
        partner = jnp.where(
            front, pltpu.roll(cells, LANES - HEAD // 2, 1), pltpu.roll(cells, HEAD // 2, 1)
        )
        return (cells * cosine + partner * sine).astype(low)

    def doubled(cells, store, t):
        turned = pltpu.roll(cells, HEAD, 1)
        store[2 * t] = jnp.where(left, cells, turned).astype(low)
        store[2 * t + 1] = jnp.where(left, turned, cells).astype(low)

    reach = pl.ds(start, span)
    for t in range(kv // LANES):
        cells = near_ref[reach, t * LANES : (t + 1) * LANES].astype(full)
        cells = rotated(cells, cos_ref[reach, :], sin_ref[reach, :]).astype(full)
        doubled(cells, kd, t)
        columns = slice(kv + t * LANES, kv + (t + 1) * LANES)
        doubled(near_ref[reach, columns].astype(full), vd, t)

    tags = near_ref[reach, 2 * kv :].astype(full)
    across = jnp.concatenate(
        [jnp.transpose(tags[i : i + step])[0:1] for i in range(0, span, step)], axis=1
    )
    gap = lax.broadcasted_iota(jnp.int32, (step, window), 1) - lax.broadcasted_iota(
        jnp.int32, (step, window), 0
    )
    band = (gap >= 0) & (gap <= 2 * step)
    for j in range(rows // step):
        mine = tags[step + j * step : 2 * step + j * step, 0:1]
        theirs = across[:, j * step : j * step + window]
        bias = jnp.where(band & (mine == theirs), 0.0, neg_large)
        at_rows = pl.ds(pl.multiple_of(start + j * step, step), step)
        mid_rows = pl.ds(pl.multiple_of(start + (j + 1) * step, step), step)
        cosine = cos_ref[mid_rows, :] * HEAD ** (-0.5)
        sine = sin_ref[mid_rows, :] * HEAD ** (-0.5)

        def one(n, carry):
            stack = []
            for t in range(2):
                columns = pl.ds(pl.multiple_of((2 * n + t) * LANES, LANES), LANES)
                cells = rotated(q_ref[at_rows, columns].astype(full), cosine, sine)
                none = jnp.zeros_like(cells)
                stack += [jnp.where(left, cells, none), jnp.where(left, none, cells)]
            keys = kd[n, j * step : j * step + window]
            scores = lax.dot_general(
                jnp.concatenate(stack, axis=0),
                keys,
                (((1,), (1,)), ((), ())),
                preferred_element_type=full,
            )
            probs = []
            shares = []
            for h in range(4):
                part = scores[h * step : (h + 1) * step] + bias
                sink = sink_ref[4 * n + h]
                top = jnp.maximum(jnp.max(part, axis=1, keepdims=True), sink)
                weights = jnp.exp(part - top)
                total = jnp.sum(weights, axis=1, keepdims=True) + jnp.exp(sink - top)
                probs.append(weights.astype(low))
                shares.append(1.0 / total)
            seen = jnp.dot(
                jnp.concatenate(probs, axis=0),
                vd[n, j * step : j * step + window],
                preferred_element_type=full,
            )
            parts = [seen[h * step : (h + 1) * step] * shares[h] for h in range(4)]
            for t in range(2):
                columns = pl.ds(pl.multiple_of((2 * n + t) * LANES, LANES), LANES)
                held[j * step : (j + 1) * step, columns] = jnp.where(
                    left, parts[2 * t], parts[2 * t + 1]
                ).astype(low)
            return carry

        lax.fori_loop(0, kv // HEAD, one, 0)
    out_ref[...] = jnp.dot(held[...], weight_ref[...], preferred_element_type=full).astype(low)


def normalize_body(core_ref, residual_ref, own_ref, given_ref, gains_ref, near_ref, updated_ref, packed_ref):
    rows, width = residual_ref.shape
    mixed = own_ref[...].astype(full) + given_ref[...].astype(full)
    updated = residual_ref[...].astype(full) + normalize(mixed, gains_ref[0:1])
    updated = updated.astype(low)
    updated_ref[...] = updated
    packed_ref[:, :width] = normalize(updated.astype(full), gains_ref[1:2]).astype(low)
    edge = 16
    start = pl.multiple_of(WINDOW - edge + core_ref[0] * rows, edge)
    tags = near_ref[pl.ds(start, rows + 2 * edge), near_ref.shape[1] - LANES :].astype(full)
    size = rows + 2 * edge
    before = pltpu.roll(tags, 1, 0)
    after = pltpu.roll(tags, size - 1, 0)
    code = jnp.where(before == tags, 1.0, 0.0) + jnp.where(after == tags, 2.0, 0.0)
    packed_ref[:, width:] = code[edge : edge + rows].astype(low)


def product_body(spots, fars, count, width, me_ref, *refs):
    tokens, pieces = refs[:count], refs[count : count + len(spots)]
    gate_ref, up_ref, whole, held, weight_sems, token_sems = refs[count + len(spots) :]
    depth = pieces[0].shape[1]
    each, rows, cells = gate_ref.shape
    at = pl.program_id(0)

    @pl.when(at == 0)
    def _():
        copies = load_rows(me_ref[0], spots, pieces, whole, weight_sems, depth, fars)
        for b in range(count):
            block = held.at[b * rows : (b + 1) * rows]
            pltpu.make_async_copy(tokens[b].at[:, :width], block, token_sems.at[b]).start()
        for copy in copies:
            copy.wait()

    for b in range(each):
        block = held.at[pl.ds(0, rows)]
        pltpu.make_async_copy(block, block, token_sems.at[at * each + b]).wait()
    start = pl.multiple_of(at * each * rows, each * rows)
    both = jnp.dot(held[pl.ds(start, each * rows)], whole[...], preferred_element_type=full)
    both = both.reshape(each, rows, 2 * cells)
    gate_ref[...] = both[:, :, :cells].astype(low)
    up_ref[...] = both[:, :, cells:]


def hidden_body(gate_ref, up_ref, code_ref, around_ref, taps_ref, own_ref, other_ref):
    each, _, rows, cells = gate_ref.shape
    for b in range(each):
        out_ref = (own_ref, other_ref)[b]
        code = code_ref[b, 0].astype(full)
        same_prev = (code == 1.0) | (code == 3.0)
        same_next = code >= 2.0
        index = lax.broadcasted_iota(jnp.int32, code.shape, 0)
        for start in range(0, cells, LANES):
            size = min(LANES, cells - start)
            columns = slice(start, start + size)
            gate = gate_ref[b, 0, :, columns].astype(full)
            top, bottom = around_ref[b, 0, 0:1, columns], around_ref[b, 0, 1:2, columns]
            at = index[:, :size]
            before = jnp.where(at == 0, top.astype(full), pltpu.roll(gate, 1, 0))
            after = jnp.where(at == rows - 1, bottom.astype(full), pltpu.roll(gate, rows - 1, 0))
            conv = (
                taps_ref[0:1, columns] * jnp.where(same_prev[:, :size], before, 0.0)
                + taps_ref[1:2, columns] * gate
                + taps_ref[2:3, columns] * jnp.where(same_next[:, :size], after, 0.0)
            )
            share = 0.5 * jnp.tanh(0.5 * conv) + 0.5
            out_ref[0, :, columns] = (conv * share * up_ref[b, 0, :, columns]).astype(low)


def down_body(spots, me_ref, *refs):
    total = 2 * len(spots)
    pieces, hiddens = refs[:total], refs[total : total + 8]
    out_refs = refs[total + 8 : total + 10]
    whole, sems = refs[total + 10 :]
    cells = pieces[0].shape[2]
    groups = len(out_refs)
    each = len(spots) // groups
    copies = [[] for _ in range(groups)]
    for half in range(2):
        for p in range(len(spots)):
            for slot in range(4):
                near = me_ref[0] ^ OFFSETS[slot]
                place = (p % each) * 4 + (near & 1) + 2 * ((near >> 2) & 1)
                columns = pl.ds(pl.multiple_of(place * cells, cells), cells)
                index = (half * len(spots) + p) * 4 + slot
                copies[p // each].append(
                    pltpu.make_async_copy(
                        pieces[half * len(spots) + p].at[slot],
                        whole.at[p // each, half, :, columns],
                        sems.at[index],
                    )
                )
    for group in copies:
        for copy in group:
            copy.start()
    for g, out_ref in enumerate(out_refs):
        for copy in copies[g]:
            copy.wait()
        picked = spots[g]
        size = cells * 4 * each // 2

        def step(i, carry):
            columns = pl.ds(pl.multiple_of(i * size, size), size)
            sums = 0.0
            for half in range(2):
                rows = []
                for b in picked:
                    first = 4 * half + 2 * (b & 1)
                    parts = [hiddens[first + c][b >> 1] for c in (0, 1)]
                    rows.append(jnp.concatenate(parts, axis=1))
                sums = sums + jnp.dot(
                    jnp.concatenate(rows, axis=0),
                    whole[g, half, :, columns],
                    preferred_element_type=full,
                )
            out_ref[:, :, columns] = sums.astype(low).reshape(len(picked), -1, size)
            return carry

        lax.fori_loop(0, 2, step, 0)


def final_body(groups, fars, me_ref, updated_ref, gain_ref, *refs):
    out_ref = refs[-1]
    me = me_ref[0]
    width = out_ref.shape[1]
    sums = []
    square = 0.0
    for g in range(len(groups)):
        own, wide, last = refs[3 * g : 3 * g + 3]
        total = own[0].astype(full) + wide[0].astype(full) + last[...].astype(full)
        square = square + jnp.sum(total * total, axis=1, keepdims=True)
        sums.append(total)
    scale = lax.rsqrt(square / width + norm_eps)
    for spots, total in zip(groups, sums):
        cells = total.shape[1] // (4 * len(spots))
        for p, (step, y) in enumerate(spots):
            for place in range(4):
                line = (me >> 1 & 1) ^ y
                far = lax.rem((me >> 3) - step + fars, fars)
                shard = far * FAR + (place >> 1) * ZL + line * Y + (place & 1)
                columns = pl.ds(pl.multiple_of(shard * cells, cells), cells)
                start = (p * 4 + place) * cells
                block = total[:, start : start + cells]
                out_ref[:, columns] = (
                    updated_ref[:, columns].astype(full) + block * scale * gain_ref[:, columns]
                ).astype(low)


def flips(cells, at):
    for axis, bit in ((0, at.core), (1, at.x), (2, at.zl)):
        cells = jnp.where(bit == 1, jnp.flip(cells, axis), cells)
    return cells


def local(
    residual_in,
    queries,
    keys,
    values,
    docs,
    sink,
    out_weight,
    gate_weight,
    up_weight,
    down_weight,
    conv_taps,
    norm_gains,
):
    at = Place()
    rows = queries.shape[0]
    own, width = residual_in.shape
    depth = gate_weight.shape[0]
    part = gate_weight.shape[1] // 4
    me = at.me.astype(jnp.int32).reshape(1)

    def columns(base, size):
        parts = [
            weight[:, i * part + base : i * part + base + size]
            for i in range(4)
            for weight in (gate_weight, up_weight)
        ]
        joined = [jnp.concatenate(parts[i : i + 2], axis=1) for i in range(0, 8, 2)]
        return jnp.stack(joined).reshape(2, 2, depth, 2 * size)

    tag = jnp.broadcast_to((docs + 1).astype(low)[:, None], (rows, LANES))
    near = jnp.concatenate([keys, values, tag], axis=1)
    line = [(i, i + 1) for i in range(at.count - 1)]
    before = lax.ppermute(near[rows - WINDOW :], "sp", line)
    after = lax.ppermute(near[:WINDOW], "sp", [(j, i) for i, j in line])

    split = -(-part // (2 * LANES)) * LANES
    sizes = (split, part - split)
    chunks = [spread(at, columns(0, sizes[0])), spread(at, columns(split, sizes[1]))]
    down_pieces = spread(at, down_weight.reshape(2, 2, part, depth))

    near = jnp.concatenate([before, near, after], axis=0)
    half = HEAD // 2
    freq = rope_base ** (-jnp.arange(half, dtype=full) * 2.0 / HEAD)
    there = at.me * rows - WINDOW + jnp.arange(rows + 2 * WINDOW, dtype=jnp.int32)
    angle = there.astype(full)[:, None] * freq[None, :]
    cosine, sine = jnp.cos(angle), jnp.sin(angle)
    cosine = jnp.concatenate([cosine] * 4, axis=1)
    sine = jnp.concatenate([-sine, sine] * 2, axis=1)

    def attended(index):
        return pl.pallas_call(
            attend_body,
            out_shape=jax.ShapeDtypeStruct((own, width), low),
            in_specs=[smem(), smem()] + [vmem()] * 5,
            out_specs=vmem(),
            scratch_shapes=[
                pltpu.VMEM((keys.shape[1] // HEAD, own + 2 * WINDOW, LANES), low),
                pltpu.VMEM((keys.shape[1] // HEAD, own + 2 * WINDOW, LANES), low),
                pltpu.VMEM((own, queries.shape[1]), low),
            ],
            compiler_params=params,
            cost_estimate=cost(9_000_000_000, 6_000_000),
        )(index, sink, queries, near, cosine, sine, out_weight)

    core = at.core.astype(jnp.int32).reshape(1)
    theirs = attended(1 - core)
    mine = attended(core)
    given = at.other_core(theirs)
    wide = width + LANES
    updated, packed = pl.pallas_call(
        normalize_body,
        out_shape=[jax.ShapeDtypeStruct((own, width), low), jax.ShapeDtypeStruct((own, wide), low)],
        in_specs=[smem()] + [vmem()] * 5,
        out_specs=[vmem()] * 2,
        compiler_params=params,
        cost_estimate=cost(2_000_000_000, 6 * own * width * 2),
        name="norm",
    )(core, residual_in, mine, given, norm_gains, near)

    by_z = swap(packed, ZL)
    by_x = swap(packed, X)
    by_xz = swap(by_z, X)
    tokens = [packed, by_z, by_x, by_xz]
    tokens += [at.other_core(block) for block in tokens]
    count = len(tokens)

    def spots(pieces):
        return tuple((step, y) for step, y, _ in pieces)

    taps = pick(conv_taps.reshape(3, 4, part), at.zl * 2 + at.x, 1)
    hops = []
    for i in range(at.count):
        goal = i - Y + FAR if i & Y else i + Y - FAR
        if 0 <= goal < at.count:
            hops.append((i, goal))

    sets = [[tokens[i] for i in (0, 2, 4, 6)], [tokens[i] for i in (1, 3, 5, 7)]]
    made = {}
    for c, (pieces, size) in enumerate(zip(chunks, sizes)):
        for t, blocks in enumerate(sets):
            made[c, t] = pl.pallas_call(
                lambda *refs: product_body(spots(pieces), at.fars, 4, width, *refs),
                out_shape=[
                    jax.ShapeDtypeStruct((4, own, size), low),
                    jax.ShapeDtypeStruct((4, own, size), full),
                ],
                grid=(2,),
                in_specs=[smem()] + [hbm()] * (4 + len(pieces)),
                out_specs=[pl.BlockSpec((2, own, size), lambda b: (b, 0, 0))] * 2,
                scratch_shapes=[
                    pltpu.VMEM((width, 2 * size), low),
                    pltpu.VMEM((4 * own, width), low),
                    pltpu.SemaphoreType.DMA((4 * len(pieces),)),
                    pltpu.SemaphoreType.DMA((4,)),
                ],
                compiler_params=params,
                cost_estimate=cost(16 * own * width * size, 8 * own * width),
            )(me, *blocks, *[piece for _, _, piece in pieces])

    def ends_of(t):
        rows_ = [jnp.concatenate([made[c, t][0][:, :1], made[c, t][0][:, -1:]], axis=1) for c in (0, 1)]
        return jnp.concatenate(rows_, axis=2).reshape(2, 2, 2, part)

    edges = jnp.stack([ends_of(0), ends_of(1)], axis=2)
    edges = flips(edges, at).transpose(2, 1, 0, 3, 4).reshape(2, 4, 2, part)
    ends = jnp.stack([edges[:, 0, 0], edges[:, 3, 1]], axis=1)
    side = swap(ends, Y)
    sent = jnp.where(at.y == 1, ends[1, 1], ends[0, 0])
    beyond = lax.ppermute(sent, "sp", hops)
    first = jnp.where(
        at.y == 1, jnp.stack([side[0, 1], side[1, 1]]), jnp.stack([beyond, side[0, 1]])
    )
    last = jnp.where(
        at.y == 1, jnp.stack([side[1, 0], beyond]), jnp.stack([side[0, 0], side[1, 0]])
    )
    prev_row = jnp.concatenate([first[:, None], edges[:, :3, 1]], axis=1)
    next_row = jnp.concatenate([edges[:, 1:, 0], last[:, None]], axis=1)
    around = jnp.stack([prev_row, next_row], axis=2).reshape(2, 2, 2, 2, part)
    around = flips(around.transpose(2, 1, 0, 3, 4), at)

    def rows_of(*cells):
        return pl.BlockSpec((2, 1) + cells, lambda b: (0, b, 0, 0))

    kept_hidden, sent_hidden = {}, {}
    for t in (0, 1):
        codes = jnp.stack([block[:, width:] for block in sets[t]]).reshape(2, 2, own, LANES)
        for c, size in enumerate(sizes):
            columns = slice(c * split, c * split + size)
            kept_hidden[c, t], sent_hidden[c, t] = pl.pallas_call(
                hidden_body,
                out_shape=[jax.ShapeDtypeStruct((2, own, size), low)] * 2,
                grid=(2,),
                in_specs=[
                    rows_of(own, size),
                    rows_of(own, size),
                    rows_of(own, LANES),
                    rows_of(2, size),
                    pl.BlockSpec((3, size), lambda b: (0, 0)),
                ],
                out_specs=[pl.BlockSpec((1, own, size), lambda b: (b, 0, 0))] * 2,
                compiler_params=params,
                cost_estimate=cost(1_500_000_000, 4 * own * size * 8),
            )(
                made[c, t][0].reshape(2, 2, own, size),
                made[c, t][1].reshape(2, 2, own, size),
                codes,
                around[:, :, t, :, columns],
                taps[:, columns],
            )

    keys_ = [(c, t) for t in (0, 1) for c in (0, 1)]
    inputs = [kept_hidden[key] for key in keys_]
    inputs += [at.other_core(sent_hidden[key]) for key in keys_]
    groups = [down_pieces[:2], down_pieces[2:]]
    cells = 4 * depth * len(groups[0])
    pieces = [piece for _, _, piece in down_pieces]
    pieces += [at.other_core(piece) for piece in pieces]

    def down(picked):
        return pl.pallas_call(
            lambda *refs: down_body(picked, *refs),
            out_shape=[jax.ShapeDtypeStruct((2, own, cells), low)] * 2,
            in_specs=[smem()] + [hbm()] * len(pieces) + [vmem()] * 8,
            out_specs=[vmem()] * 2,
            scratch_shapes=[
                pltpu.VMEM((2, 2, part, cells), low),
                pltpu.SemaphoreType.DMA((4 * len(pieces),)),
            ],
            compiler_params=params,
            cost_estimate=cost(count * own * part * width, 6 * own * width),
        )(me, *pieces, *inputs)

    sent_x, sent_z = down(((2, 3), (1, 3), (), ()))
    kept_x, kept_z = down(((0, 1), (0, 2), (), ()))
    wide_x = swap(sent_x, X)
    wide_z = swap(sent_z, ZL)
    finals = []
    for kept, wide_sum, bit in ((kept_x, wide_x, ZL), (kept_z, wide_z, X)):
        sent = (kept[1].astype(full) + wide_sum[1].astype(full)).astype(low)
        finals += [kept, wide_sum, swap(sent, bit)]

    def blocks(i):
        cells = finals[i].shape[-1]
        if i % 3 == 2:
            return pl.BlockSpec((own // 4, cells), lambda s: (s, 0))
        return pl.BlockSpec((1, own // 4, cells), lambda s: (0, s, 0))

    whole = pl.BlockSpec((own // 4, width), lambda s: (s, 0))
    return pl.pallas_call(
        lambda *refs: final_body([spots(pieces) for pieces in groups], at.fars, *refs),
        out_shape=jax.ShapeDtypeStruct((own, width), low),
        grid=(4,),
        in_specs=[smem(), whole, pl.BlockSpec((1, width), lambda s: (0, 0))]
        + [blocks(i) for i in range(len(finals))],
        out_specs=whole,
        compiler_params=params,
        cost_estimate=cost(own * width * 10, own * width * 14),
        name="final",
    )(me, updated, norm_gains[2:3], *finals)


def grouped(mesh, shapes):
    sp, tp = mesh.shape["sp"], mesh.shape["tp"]
    width, hidden = shapes[7].shape
    fits = tp == 2 and sp == 2 * FAR
    return fits and width // sp % LANES == 0 and hidden // tp // 4 % 16 == 0


def staged(*arrays):
    return local(*arrays)


def solution(mesh):
    in_specs = (
        P(("sp", "tp"), None),
        P("sp", "tp"),
        P("sp", "tp"),
        P("sp", "tp"),
        P("sp"),
        P("tp"),
        P("tp", None),
        P("sp", "tp"),
        P("sp", "tp"),
        P("tp", "sp"),
        P(None, "tp"),
        P(),
    )
    out_specs = P(("sp", "tp"), None)

    def run(*arrays):
        fits = grouped(mesh, arrays)
        step = jax.shard_map(
            staged if fits else plain,
            mesh=mesh,
            in_specs=in_specs,
            out_specs=out_specs,
            check_vma=False,
        )
        return step(*arrays)

    return run
```

```python
import jax
import jax.numpy as jnp
from jax import lax
from jax.experimental import pallas as pl
from jax.experimental.pallas import tpu as pltpu
from jax.sharding import PartitionSpec as P


HEAD = 64
WINDOW = 128


rope_base = 10000.0
neg_large = -1e30
norm_eps = 1e-06


def padded(cells, sides, width):
    for axis, dim in sides:
        count = lax.axis_size(axis)
        ends = count - 1
        head = lax.slice_in_dim(cells, 0, width, axis=dim)
        tail = lax.slice_in_dim(cells, cells.shape[dim] - width, cells.shape[dim], axis=dim)
        cells = jnp.concatenate(
            [
                lax.ppermute(tail, axis, [(i, (i + 1) % count) for i in range(ends)]),
                cells,
                lax.ppermute(head, axis, [((i + 1) % count, i) for i in range(ends)]),
            ],
            axis=dim,
        )
    return cells


def rotate(block, positions):
    rows = block.shape[0]
    heads = block.shape[1] // HEAD
    half = HEAD // 2
    freq = rope_base ** (-jnp.arange(half, dtype=jnp.float32) * 2.0 / HEAD)
    angle = positions.astype(jnp.float32)[:, None] * freq[None, :]
    cosine = jnp.cos(angle)[:, None, :]
    sine = jnp.sin(angle)[:, None, :]
    shaped = block.astype(jnp.float32).reshape(rows, heads, 2, half)
    first = shaped[:, :, 0]
    second = shaped[:, :, 1]
    turned = jnp.stack([first * cosine - second * sine, second * cosine + first * sine], axis=2)
    return turned.reshape(rows, heads * HEAD).astype(jnp.bfloat16)


def attend(queries, keys, values, allowed, sink):
    rows = queries.shape[0]
    kv_local = keys.shape[1] // HEAD
    group = queries.shape[1] // HEAD // kv_local
    shaped_q = queries.reshape(rows, kv_local, group, HEAD)
    shaped_k = keys.reshape(keys.shape[0], kv_local, HEAD)
    shaped_v = values.reshape(values.shape[0], kv_local, HEAD)
    scores = jnp.einsum(
        "qngd,knd->ngqk", shaped_q, shaped_k, preferred_element_type=jnp.float32
    ) * HEAD ** (-0.5)
    scores = jnp.where(allowed[None, None], scores, neg_large)
    sink_group = sink.reshape(kv_local, group)[:, :, None]
    top = jnp.maximum(jnp.max(scores, axis=-1), sink_group)
    weights = jnp.exp(scores - top[..., None])
    total = jnp.sum(weights, axis=-1) + jnp.exp(sink_group - top)
    probs = (weights / total[..., None]).astype(jnp.bfloat16)
    out = jnp.einsum("ngqk,knd->qngd", probs, shaped_v, preferred_element_type=jnp.float32)
    return out.reshape(rows, kv_local * group * HEAD).astype(jnp.bfloat16)


def normalize(vector, gain):
    scale = lax.rsqrt(jnp.mean(vector * vector, axis=-1, keepdims=True) + norm_eps)
    return vector * scale * gain


def plain(
    residual_in,
    queries,
    keys,
    values,
    docs,
    sink,
    out_weight,
    gate_weight,
    up_weight,
    down_weight,
    conv_taps,
    norm_gains,
):
    rows = queries.shape[0]
    offset = lax.axis_index("sp") * rows
    total_len = lax.axis_size("sp") * rows
    keys_ext, values_ext, docs_ext = (
        padded(keys, (("sp", 0),), WINDOW),
        padded(values, (("sp", 0),), WINDOW),
        padded(docs, (("sp", 0),), WINDOW),
    )
    here = offset + jnp.arange(rows, dtype=jnp.int32)
    there = offset - WINDOW + jnp.arange(rows + 2 * WINDOW, dtype=jnp.int32)
    q_rot = rotate(queries, here)
    k_rot = rotate(keys_ext, there)
    allowed = (
        (jnp.abs(there[None, :] - here[:, None]) <= WINDOW)
        & (there[None, :] >= 0)
        & (there[None, :] < total_len)
        & (docs_ext[None, :] == docs[:, None])
    )
    attended = attend(q_rot, k_rot, values_ext, allowed, sink)
    mixed = lax.psum_scatter(
        jnp.dot(attended, out_weight, preferred_element_type=jnp.float32).astype(jnp.bfloat16),
        "tp",
        scatter_dimension=0,
        tiled=True,
    ).astype(jnp.float32)
    updated = (residual_in.astype(jnp.float32) + normalize(mixed, norm_gains[0])).astype(
        jnp.bfloat16
    )
    normed = normalize(updated.astype(jnp.float32), norm_gains[1]).astype(jnp.bfloat16)
    ffn_in = lax.all_gather(normed, "tp", axis=0, tiled=True)
    gate = jnp.dot(
        ffn_in,
        lax.all_gather(gate_weight, "sp", axis=0, tiled=True),
        preferred_element_type=jnp.float32,
    )
    up = jnp.dot(
        ffn_in,
        lax.all_gather(up_weight, "sp", axis=0, tiled=True),
        preferred_element_type=jnp.float32,
    )
    gate_low = gate.astype(jnp.bfloat16)
    gate_ext = padded(gate_low, (("sp", 0),), 1).astype(jnp.float32)
    same_prev = (docs_ext[WINDOW - 1 : WINDOW - 1 + rows] == docs)[:, None]
    same_next = (docs_ext[WINDOW + 1 : WINDOW + 1 + rows] == docs)[:, None]
    conv = (
        conv_taps[0] * jnp.where(same_prev, gate_ext[:-2], 0.0)
        + conv_taps[1] * gate_ext[1:-1]
        + conv_taps[2] * jnp.where(same_next, gate_ext[2:], 0.0)
    )
    hidden = (jax.nn.silu(conv) * up).astype(jnp.bfloat16)
    terms = jnp.dot(
        hidden,
        lax.all_gather(down_weight, "sp", axis=1, tiled=True),
        preferred_element_type=jnp.float32,
    )
    ffn_out = lax.psum_scatter(
        terms.astype(jnp.bfloat16), "tp", scatter_dimension=0, tiled=True
    ).astype(jnp.float32)
    return (updated.astype(jnp.float32) + normalize(ffn_out, norm_gains[2])).astype(jnp.bfloat16)


LANES = 128
X, Y, ZL, FAR = 1, 2, 4, 8
low = jnp.bfloat16
full = jnp.float32
params = pltpu.CompilerParams(vmem_limit_bytes=60 * 1024 * 1024)


def hbm():
    return pl.BlockSpec(memory_space=pl.ANY)


def vmem():
    return pl.BlockSpec(memory_space=pltpu.VMEM)


def smem():
    return pl.BlockSpec(memory_space=pltpu.SMEM)


def cost(flops, bytes_accessed):
    return pl.CostEstimate(flops=flops, bytes_accessed=bytes_accessed, transcendentals=0)


def swap(cells, bit):
    return lax.ppermute(cells, "sp", [(i, i ^ bit) for i in range(lax.axis_size("sp"))])


def pick(cells, index, axis):
    return lax.dynamic_index_in_dim(cells, index, axis, keepdims=False)


class Place:
    def __init__(self):
        self.me = lax.axis_index("sp")
        self.core = lax.axis_index("tp")
        self.count = lax.axis_size("sp")
        self.cores = lax.axis_size("tp")
        self.x = self.me & 1
        self.y = (self.me >> 1) & 1
        self.zl = (self.me >> 2) & 1
        self.fars = self.count // FAR

    def other_core(self, cells):
        return lax.ppermute(cells, "tp", [(i, i ^ 1) for i in range(self.cores)])

    def far_shift(self, cells, step):
        hops = [(i, (i + step * FAR) % self.count) for i in range(self.count)]
        return lax.ppermute(cells, "sp", hops)


def exchange(at, parts):
    kept = pick(parts, at.x, 1)
    came = swap(pick(parts, 1 - at.x, 1), X)
    sent = jnp.stack([pick(kept, 1 - at.zl, 0), pick(came, 1 - at.zl, 0)])
    mine = jnp.stack([pick(kept, at.zl, 0), pick(came, at.zl, 0)])
    return jnp.concatenate([mine, swap(sent, ZL)])


def spread(at, parts):
    four = exchange(at, parts)
    pieces = [(0, 0, four), (0, 1, swap(four, Y))]
    for step in range(1, at.fars):
        away = at.far_shift(four, step)
        pieces += [(step, 0, away), (step, 1, swap(away, Y))]
    return pieces


OFFSETS = (0, X, ZL, X | ZL)


def shard_of(me, fars, step, y, slot):
    near = (me & 7) ^ (OFFSETS[slot] | (Y if y else 0))
    return near + FAR * lax.rem((me >> 3) - step + fars, fars)


def load_rows(me, spots, refs, whole, sems, depth, fars):
    copies = []
    for (step, y), ref in zip(spots, refs):
        for slot in range(4):
            shard = shard_of(me, fars, step, y, slot)
            rows = pl.ds(pl.multiple_of(shard * depth, depth), depth)
            copies.append(
                pltpu.make_async_copy(ref.at[slot], whole.at[rows], sems.at[len(copies)])
            )
    for copy in copies:
        copy.start()
    return copies


def attend_body(half_ref, sink_ref, q_ref, near_ref, cos_ref, sin_ref, weight_ref, out_ref, kd, vd, held):
    kv = held.shape[1] // 4
    span = kd.shape[1]
    rows = held.shape[0]
    step = WINDOW
    window = 3 * step
    start = pl.multiple_of(half_ref[0] * rows, rows)
    lane = lax.broadcasted_iota(jnp.int32, (1, LANES), 1)
    front = lane % HEAD < HEAD // 2
    left = lane < HEAD

    def rotated(cells, cosine, sine):
        partner = jnp.where(
            front, pltpu.roll(cells, LANES - HEAD // 2, 1), pltpu.roll(cells, HEAD // 2, 1)
        )
        return (cells * cosine + partner * sine).astype(low)

    def doubled(cells, store, t):
        turned = pltpu.roll(cells, HEAD, 1)
        store[2 * t] = jnp.where(left, cells, turned).astype(low)
        store[2 * t + 1] = jnp.where(left, turned, cells).astype(low)

    reach = pl.ds(start, span)
    for t in range(kv // LANES):
        cells = near_ref[reach, t * LANES : (t + 1) * LANES].astype(full)
        cells = rotated(cells, cos_ref[reach, :], sin_ref[reach, :]).astype(full)
        doubled(cells, kd, t)
        columns = slice(kv + t * LANES, kv + (t + 1) * LANES)
        doubled(near_ref[reach, columns].astype(full), vd, t)

    tags = near_ref[reach, 2 * kv :].astype(full)
    across = jnp.concatenate(
        [jnp.transpose(tags[i : i + step])[0:1] for i in range(0, span, step)], axis=1
    )
    gap = lax.broadcasted_iota(jnp.int32, (step, window), 1) - lax.broadcasted_iota(
        jnp.int32, (step, window), 0
    )
    band = (gap >= 0) & (gap <= 2 * step)
    for j in range(rows // step):
        mine = tags[step + j * step : 2 * step + j * step, 0:1]
        theirs = across[:, j * step : j * step + window]
        bias = jnp.where(band & (mine == theirs), 0.0, neg_large)
        at_rows = pl.ds(pl.multiple_of(start + j * step, step), step)
        mid_rows = pl.ds(pl.multiple_of(start + (j + 1) * step, step), step)
        cosine = cos_ref[mid_rows, :] * HEAD ** (-0.5)
        sine = sin_ref[mid_rows, :] * HEAD ** (-0.5)

        def one(n, carry):
            stack = []
            for t in range(2):
                columns = pl.ds(pl.multiple_of((2 * n + t) * LANES, LANES), LANES)
                cells = rotated(q_ref[at_rows, columns].astype(full), cosine, sine)
                none = jnp.zeros_like(cells)
                stack += [jnp.where(left, cells, none), jnp.where(left, none, cells)]
            keys = kd[n, j * step : j * step + window]
            scores = lax.dot_general(
                jnp.concatenate(stack, axis=0),
                keys,
                (((1,), (1,)), ((), ())),
                preferred_element_type=full,
            )
            probs = []
            shares = []
            for h in range(4):
                part = scores[h * step : (h + 1) * step] + bias
                sink = sink_ref[4 * n + h]
                top = jnp.maximum(jnp.max(part, axis=1, keepdims=True), sink)
                weights = jnp.exp(part - top)
                total = jnp.sum(weights, axis=1, keepdims=True) + jnp.exp(sink - top)
                probs.append(weights.astype(low))
                shares.append(1.0 / total)
            seen = jnp.dot(
                jnp.concatenate(probs, axis=0),
                vd[n, j * step : j * step + window],
                preferred_element_type=full,
            )
            parts = [seen[h * step : (h + 1) * step] * shares[h] for h in range(4)]
            for t in range(2):
                columns = pl.ds(pl.multiple_of((2 * n + t) * LANES, LANES), LANES)
                held[j * step : (j + 1) * step, columns] = jnp.where(
                    left, parts[2 * t], parts[2 * t + 1]
                ).astype(low)
            return carry

        lax.fori_loop(0, kv // HEAD, one, 0)
    out_ref[...] = jnp.dot(held[...], weight_ref[...], preferred_element_type=full).astype(low)


def normalize_body(core_ref, residual_ref, own_ref, given_ref, gains_ref, near_ref, updated_ref, packed_ref):
    rows, width = residual_ref.shape
    mixed = own_ref[...].astype(full) + given_ref[...].astype(full)
    updated = residual_ref[...].astype(full) + normalize(mixed, gains_ref[0:1])
    updated = updated.astype(low)
    updated_ref[...] = updated
    packed_ref[:, :width] = normalize(updated.astype(full), gains_ref[1:2]).astype(low)
    edge = 16
    start = pl.multiple_of(WINDOW - edge + core_ref[0] * rows, edge)
    tags = near_ref[pl.ds(start, rows + 2 * edge), near_ref.shape[1] - LANES :].astype(full)
    size = rows + 2 * edge
    before = pltpu.roll(tags, 1, 0)
    after = pltpu.roll(tags, size - 1, 0)
    code = jnp.where(before == tags, 1.0, 0.0) + jnp.where(after == tags, 2.0, 0.0)
    packed_ref[:, width:] = code[edge : edge + rows].astype(low)


def product_body(spots, fars, count, width, me_ref, *refs):
    tokens, pieces = refs[:count], refs[count : count + len(spots)]
    gate_ref, up_ref, whole, held, weight_sems, token_sems = refs[count + len(spots) :]
    depth = pieces[0].shape[1]
    each, rows, cells = gate_ref.shape
    at = pl.program_id(0)

    @pl.when(at == 0)
    def _():
        copies = load_rows(me_ref[0], spots, pieces, whole, weight_sems, depth, fars)
        for b in range(count):
            block = held.at[b * rows : (b + 1) * rows]
            pltpu.make_async_copy(tokens[b].at[:, :width], block, token_sems.at[b]).start()
        for copy in copies:
            copy.wait()

    for b in range(each):
        block = held.at[pl.ds(0, rows)]
        pltpu.make_async_copy(block, block, token_sems.at[at * each + b]).wait()
    start = pl.multiple_of(at * each * rows, each * rows)
    both = jnp.dot(held[pl.ds(start, each * rows)], whole[...], preferred_element_type=full)
    both = both.reshape(each, rows, 2 * cells)
    gate_ref[...] = both[:, :, :cells].astype(low)
    up_ref[...] = both[:, :, cells:]


def hidden_body(gate_ref, up_ref, code_ref, around_ref, taps_ref, own_ref, other_ref):
    _, each, _, rows, cells = gate_ref.shape
    for b in range(each):
        out_ref = (own_ref, other_ref)[b]
        code = code_ref[b, 0].astype(full)
        same_prev = (code == 1.0) | (code == 3.0)
        same_next = code >= 2.0
        index = lax.broadcasted_iota(jnp.int32, code.shape, 0)
        for start in range(0, cells, LANES):
            size = min(LANES, cells - start)
            columns = slice(start, start + size)
            gate = gate_ref[0, b, 0, :, columns].astype(full)
            top, bottom = around_ref[b, 0, 0:1, columns], around_ref[b, 0, 1:2, columns]
            at = index[:, :size]
            before = jnp.where(at == 0, top.astype(full), pltpu.roll(gate, 1, 0))
            after = jnp.where(at == rows - 1, bottom.astype(full), pltpu.roll(gate, rows - 1, 0))
            conv = (
                taps_ref[0:1, columns] * jnp.where(same_prev[:, :size], before, 0.0)
                + taps_ref[1:2, columns] * gate
                + taps_ref[2:3, columns] * jnp.where(same_next[:, :size], after, 0.0)
            )
            share = 0.5 * jnp.tanh(0.5 * conv) + 0.5
            out_ref[0, :, columns] = (conv * share * up_ref[0, b, 0, :, columns]).astype(low)


def down_body(spots, me_ref, *refs):
    total = 2 * len(spots)
    pieces, hiddens = refs[:total], refs[total : total + 8]
    out_refs = refs[total + 8 : total + 10]
    whole, sems = refs[total + 10 :]
    cells = pieces[0].shape[2]
    groups = len(out_refs)
    each = len(spots) // groups
    copies = [[] for _ in range(groups)]
    for half in range(2):
        for p in range(len(spots)):
            for slot in range(4):
                near = me_ref[0] ^ OFFSETS[slot]
                place = (p % each) * 4 + (near & 1) + 2 * ((near >> 2) & 1)
                columns = pl.ds(pl.multiple_of(place * cells, cells), cells)
                index = (half * len(spots) + p) * 4 + slot
                copies[p // each].append(
                    pltpu.make_async_copy(
                        pieces[half * len(spots) + p].at[slot],
                        whole.at[p // each, half, :, columns],
                        sems.at[index],
                    )
                )
    for group in copies:
        for copy in group:
            copy.start()
    for g, out_ref in enumerate(out_refs):
        for copy in copies[g]:
            copy.wait()
        picked = spots[g]
        size = cells * 4 * each // 2

        def step(i, carry):
            columns = pl.ds(pl.multiple_of(i * size, size), size)
            sums = 0.0
            for half in range(2):
                rows = []
                for b in picked:
                    first = 4 * half + 2 * (b & 1)
                    parts = [hiddens[first + c][b >> 1] for c in (0, 1)]
                    rows.append(jnp.concatenate(parts, axis=1))
                sums = sums + jnp.dot(
                    jnp.concatenate(rows, axis=0),
                    whole[g, half, :, columns],
                    preferred_element_type=full,
                )
            out_ref[:, :, columns] = sums.astype(low).reshape(len(picked), -1, size)
            return carry

        lax.fori_loop(0, 2, step, 0)


def final_body(groups, fars, me_ref, updated_ref, gain_ref, *refs):
    out_ref = refs[-1]
    me = me_ref[0]
    width = out_ref.shape[1]
    sums = []
    square = 0.0
    for g in range(len(groups)):
        own, wide, last = refs[3 * g : 3 * g + 3]
        total = own[0].astype(full) + wide[0].astype(full) + last[...].astype(full)
        square = square + jnp.sum(total * total, axis=1, keepdims=True)
        sums.append(total)
    scale = lax.rsqrt(square / width + norm_eps)
    for spots, total in zip(groups, sums):
        cells = total.shape[1] // (4 * len(spots))
        for p, (step, y) in enumerate(spots):
            for place in range(4):
                line = (me >> 1 & 1) ^ y
                far = lax.rem((me >> 3) - step + fars, fars)
                shard = far * FAR + (place >> 1) * ZL + line * Y + (place & 1)
                columns = pl.ds(pl.multiple_of(shard * cells, cells), cells)
                start = (p * 4 + place) * cells
                block = total[:, start : start + cells]
                out_ref[:, columns] = (
                    updated_ref[:, columns].astype(full) + block * scale * gain_ref[:, columns]
                ).astype(low)


def flips(cells, at):
    for axis, bit in ((0, at.core), (1, at.x), (2, at.zl)):
        cells = jnp.where(bit == 1, jnp.flip(cells, axis), cells)
    return cells


def local(
    residual_in,
    queries,
    keys,
    values,
    docs,
    sink,
    out_weight,
    gate_weight,
    up_weight,
    down_weight,
    conv_taps,
    norm_gains,
):
    at = Place()
    rows = queries.shape[0]
    own, width = residual_in.shape
    depth = gate_weight.shape[0]
    part = gate_weight.shape[1] // 4
    me = at.me.astype(jnp.int32).reshape(1)

    def columns(base, size):
        parts = [
            weight[:, i * part + base : i * part + base + size]
            for i in range(4)
            for weight in (gate_weight, up_weight)
        ]
        joined = [jnp.concatenate(parts[i : i + 2], axis=1) for i in range(0, 8, 2)]
        return jnp.stack(joined).reshape(2, 2, depth, 2 * size)

    tag = jnp.broadcast_to((docs + 1).astype(low)[:, None], (rows, LANES))
    near = jnp.concatenate([keys, values, tag], axis=1)
    line = [(i, i + 1) for i in range(at.count - 1)]
    before = lax.ppermute(near[rows - WINDOW :], "sp", line)
    after = lax.ppermute(near[:WINDOW], "sp", [(j, i) for i, j in line])

    split = -(-part // (2 * LANES)) * LANES
    sizes = (split, part - split)
    chunks = [spread(at, columns(0, sizes[0])), spread(at, columns(split, sizes[1]))]
    down_pieces = spread(at, down_weight.reshape(2, 2, part, depth))

    near = jnp.concatenate([before, near, after], axis=0)
    half = HEAD // 2
    freq = rope_base ** (-jnp.arange(half, dtype=full) * 2.0 / HEAD)
    there = at.me * rows - WINDOW + jnp.arange(rows + 2 * WINDOW, dtype=jnp.int32)
    angle = there.astype(full)[:, None] * freq[None, :]
    cosine, sine = jnp.cos(angle), jnp.sin(angle)
    cosine = jnp.concatenate([cosine] * 4, axis=1)
    sine = jnp.concatenate([-sine, sine] * 2, axis=1)

    def attended(index):
        return pl.pallas_call(
            attend_body,
            out_shape=jax.ShapeDtypeStruct((own, width), low),
            in_specs=[smem(), smem()] + [vmem()] * 5,
            out_specs=vmem(),
            scratch_shapes=[
                pltpu.VMEM((keys.shape[1] // HEAD, own + 2 * WINDOW, LANES), low),
                pltpu.VMEM((keys.shape[1] // HEAD, own + 2 * WINDOW, LANES), low),
                pltpu.VMEM((own, queries.shape[1]), low),
            ],
            compiler_params=params,
            cost_estimate=cost(9_000_000_000, 6_000_000),
        )(index, sink, queries, near, cosine, sine, out_weight)

    core = at.core.astype(jnp.int32).reshape(1)
    theirs = attended(1 - core)
    mine = attended(core)
    given = at.other_core(theirs)
    wide = width + LANES
    updated, packed = pl.pallas_call(
        normalize_body,
        out_shape=[jax.ShapeDtypeStruct((own, width), low), jax.ShapeDtypeStruct((own, wide), low)],
        in_specs=[smem()] + [vmem()] * 5,
        out_specs=[vmem()] * 2,
        compiler_params=params,
        cost_estimate=cost(2_000_000_000, 6 * own * width * 2),
        name="norm",
    )(core, residual_in, mine, given, norm_gains, near)

    by_z = swap(packed, ZL)
    by_x = swap(packed, X)
    by_xz = swap(by_z, X)
    tokens = [packed, by_z, by_x, by_xz]
    tokens += [at.other_core(block) for block in tokens]
    count = len(tokens)

    def spots(pieces):
        return tuple((step, y) for step, y, _ in pieces)

    taps = pick(conv_taps.reshape(3, 4, part), at.zl * 2 + at.x, 1)
    hops = []
    for i in range(at.count):
        goal = i - Y + FAR if i & Y else i + Y - FAR
        if 0 <= goal < at.count:
            hops.append((i, goal))

    sets = [[tokens[i] for i in (0, 2, 4, 6)], [tokens[i] for i in (1, 3, 5, 7)]]

    def products(c, blocks):
        pieces, size = chunks[c], sizes[c]
        number = len(blocks)
        gate, up = pl.pallas_call(
            lambda *refs: product_body(spots(pieces), at.fars, number, width, *refs),
            out_shape=[
                jax.ShapeDtypeStruct((number, own, size), low),
                jax.ShapeDtypeStruct((number, own, size), full),
            ],
            grid=(number // 2,),
            in_specs=[smem()] + [hbm()] * (number + len(pieces)),
            out_specs=[pl.BlockSpec((2, own, size), lambda b: (b, 0, 0))] * 2,
            scratch_shapes=[
                pltpu.VMEM((width, 2 * size), low),
                pltpu.VMEM((number * own, width), low),
                pltpu.SemaphoreType.DMA((4 * len(pieces),)),
                pltpu.SemaphoreType.DMA((number,)),
            ],
            compiler_params=params,
            cost_estimate=cost(4 * number * own * width * size, 2 * number * own * width),
        )(me, *blocks, *[piece for _, _, piece in pieces])
        return gate.reshape(-1, 2, 2, own, size), up.reshape(-1, 2, 2, own, size)

    both = products(1, sets[0] + sets[1])
    made = {(1, 0): (both, 0), (1, 1): (both, 1)}
    for t in (0, 1):
        made[0, t] = (products(0, sets[t]), 0)

    def ends_of(t):
        gates = [made[c, t][0][0][made[c, t][1]] for c in (0, 1)]
        rows_ = [jnp.concatenate([gate[:, :, :1], gate[:, :, -1:]], axis=2) for gate in gates]
        return jnp.concatenate(rows_, axis=3)

    edges = jnp.stack([ends_of(0), ends_of(1)], axis=2)
    edges = flips(edges, at).transpose(2, 1, 0, 3, 4).reshape(2, 4, 2, part)
    ends = jnp.stack([edges[:, 0, 0], edges[:, 3, 1]], axis=1)
    side = swap(ends, Y)
    sent = jnp.where(at.y == 1, ends[1, 1], ends[0, 0])
    beyond = lax.ppermute(sent, "sp", hops)
    first = jnp.where(
        at.y == 1, jnp.stack([side[0, 1], side[1, 1]]), jnp.stack([beyond, side[0, 1]])
    )
    last = jnp.where(
        at.y == 1, jnp.stack([side[1, 0], beyond]), jnp.stack([side[0, 0], side[1, 0]])
    )
    prev_row = jnp.concatenate([first[:, None], edges[:, :3, 1]], axis=1)
    next_row = jnp.concatenate([edges[:, 1:, 0], last[:, None]], axis=1)
    around = jnp.stack([prev_row, next_row], axis=2).reshape(2, 2, 2, 2, part)
    around = flips(around.transpose(2, 1, 0, 3, 4), at)

    def rows_of(*cells):
        return pl.BlockSpec((2, 1) + cells, lambda b: (0, b, 0, 0))

    kept_hidden, sent_hidden = {}, {}
    for t in (0, 1):
        codes = jnp.stack([block[:, width:] for block in sets[t]]).reshape(2, 2, own, LANES)
        for c, size in enumerate(sizes):
            columns = slice(c * split, c * split + size)
            (gate, up), place = made[c, t]
            spec = pl.BlockSpec((1, 2, 1, own, size), lambda b, k=place: (k, 0, b, 0, 0))
            kept_hidden[c, t], sent_hidden[c, t] = pl.pallas_call(
                hidden_body,
                out_shape=[jax.ShapeDtypeStruct((2, own, size), low)] * 2,
                grid=(2,),
                in_specs=[
                    spec,
                    spec,
                    rows_of(own, LANES),
                    rows_of(2, size),
                    pl.BlockSpec((3, size), lambda b: (0, 0)),
                ],
                out_specs=[pl.BlockSpec((1, own, size), lambda b: (b, 0, 0))] * 2,
                compiler_params=params,
                cost_estimate=cost(1_500_000_000, 4 * own * size * 8),
            )(
                gate,
                up,
                codes,
                around[:, :, t, :, columns],
                taps[:, columns],
            )

    keys_ = [(c, t) for t in (0, 1) for c in (0, 1)]
    inputs = [kept_hidden[key] for key in keys_]
    inputs += [at.other_core(sent_hidden[key]) for key in keys_]
    groups = [down_pieces[:2], down_pieces[2:]]
    cells = 4 * depth * len(groups[0])
    pieces = [piece for _, _, piece in down_pieces]
    pieces += [at.other_core(piece) for piece in pieces]

    def down(picked):
        return pl.pallas_call(
            lambda *refs: down_body(picked, *refs),
            out_shape=[jax.ShapeDtypeStruct((2, own, cells), low)] * 2,
            in_specs=[smem()] + [hbm()] * len(pieces) + [vmem()] * 8,
            out_specs=[vmem()] * 2,
            scratch_shapes=[
                pltpu.VMEM((2, 2, part, cells), low),
                pltpu.SemaphoreType.DMA((4 * len(pieces),)),
            ],
            compiler_params=params,
            cost_estimate=cost(count * own * part * width, 6 * own * width),
        )(me, *pieces, *inputs)

    sent_x, sent_z = down(((2, 3), (1, 3), (), ()))
    kept_x, kept_z = down(((0, 1), (0, 2), (), ()))
    wide_x = swap(sent_x, X)
    wide_z = swap(sent_z, ZL)
    finals = []
    for kept, wide_sum, bit in ((kept_x, wide_x, ZL), (kept_z, wide_z, X)):
        sent = (kept[1].astype(full) + wide_sum[1].astype(full)).astype(low)
        finals += [kept, wide_sum, swap(sent, bit)]

    def blocks(i):
        cells = finals[i].shape[-1]
        if i % 3 == 2:
            return pl.BlockSpec((own // 4, cells), lambda s: (s, 0))
        return pl.BlockSpec((1, own // 4, cells), lambda s: (0, s, 0))

    whole = pl.BlockSpec((own // 4, width), lambda s: (s, 0))
    return pl.pallas_call(
        lambda *refs: final_body([spots(pieces) for pieces in groups], at.fars, *refs),
        out_shape=jax.ShapeDtypeStruct((own, width), low),
        grid=(4,),
        in_specs=[smem(), whole, pl.BlockSpec((1, width), lambda s: (0, 0))]
        + [blocks(i) for i in range(len(finals))],
        out_specs=whole,
        compiler_params=params,
        cost_estimate=cost(own * width * 10, own * width * 14),
        name="final",
    )(me, updated, norm_gains[2:3], *finals)


def grouped(mesh, shapes):
    sp, tp = mesh.shape["sp"], mesh.shape["tp"]
    width, hidden = shapes[7].shape
    fits = tp == 2 and sp == 2 * FAR
    return fits and width // sp % LANES == 0 and hidden // tp // 4 % 16 == 0


def staged(*arrays):
    return local(*arrays)


def solution(mesh):
    in_specs = (
        P(("sp", "tp"), None),
        P("sp", "tp"),
        P("sp", "tp"),
        P("sp", "tp"),
        P("sp"),
        P("tp"),
        P("tp", None),
        P("sp", "tp"),
        P("sp", "tp"),
        P("tp", "sp"),
        P(None, "tp"),
        P(),
    )
    out_specs = P(("sp", "tp"), None)

    def run(*arrays):
        fits = grouped(mesh, arrays)
        step = jax.shard_map(
            staged if fits else plain,
            mesh=mesh,
            in_specs=in_specs,
            out_specs=out_specs,
            check_vma=False,
        )
        return step(*arrays)

    return run
```
